32 devices in a mesh: sp: 4 (over z), fs: 4 (over y, x), tp: 2 (over core).
Axes of the slice: x: 2, y: 2, z: 4, core: 2. Of those that a mesh axis runs over, the one named last changes fastest.
Arguments:
- tokens: bfloat16 [4096, 2048], P(('fs', 'sp', 'tp')), parts along dimension 0, may hold values from -6 to 6
- norm_gain: float32 [2048], replicated, may hold values from 0.1 to 1.9
- recurrent_input: bfloat16 [2048, 1024], P(None, 'tp'), may hold values from -0.125 to 0.125
- recurrent_gate: bfloat16 [2048, 1024], P(None, 'tp'), may hold values from -0.125 to 0.125
- attention_gate: bfloat16 [2048, 1024], P(None, 'tp'), may hold values from -0.125 to 0.125
- query_proj: bfloat16 [2048, 1536], P(None, 'tp'), may hold values from -0.125 to 0.125
- latent_down: bfloat16 [2048, 512], P(None, 'tp'), may hold values from -0.125 to 0.125
- rope_key_down: bfloat16 [2048, 64], replicated, may hold values from -0.125 to 0.125
- conv_kernel: float32 [4, 1024], P(None, 'tp'), may hold values from -3 to 3
- recurrence_gate_blocks: bfloat16 [16, 64, 64], P('tp'), may hold values from -0.75 to 0.75
- input_gate_blocks: bfloat16 [16, 64, 64], P('tp'), may hold values from -0.75 to 0.75
- decay_rate: float32 [1024], P('tp'), as said below
- decay_shift: float32 [4096], P(('fs', 'sp')), parts along dimension 0, may hold values from -2 to 0, as said below
- initial_state: float32 [4096], P(('fs', 'tp')), parts along dimension 0, may hold values from -6 to 6
- latent_gain: float32 [512], replicated, may hold values from 0.1 to 1.9
- latent_up: bfloat16 [512, 2048], P(None, 'tp'), may hold values from -0.25 to 0.25
- query_gain: float32 [192], replicated, may hold values from 0.4 to 250, as said below
- recurrent_output: bfloat16 [1024, 2048], P('tp'), may hold values from -0.25 to 0.25
- attention_output: bfloat16 [1024, 2048], P('tp'), may hold values from -0.25 to 0.25
Outputs:
- mixed_output: bfloat16 [4096, 2048], P(('fs', 'sp', 'tp')), parts along dimension 0
The draws below stay inside these ranges and needn't reach their ends.
There are 4 independent parts, one for each index of `fs`. The reference program is written for one: setup_inputs(seed, part) draws one part's arguments, and reference() takes and returns one part's arrays. A program takes and returns all parts, laid end to end along the dimension named above; an argument that names none is the same for every part. Nothing has to cross between parts.
Inputs may be any that keep to these rules, and one draw needn't show every extreme that they name: `decay_rate`: positive. `decay_shift`: negative. `query_gain`: positive.
All inputs are finite; a program needn't handle non-finite values.
Results may differ from the reference program's by a relative error of at most 0.03.
The reference program's roundings to bfloat16 on the way count: a program that leaves them out, or rounds other values in their place, can miss the bound.
Values may be sent and summed in bfloat16 or wider, within the bound.
No kernel may reach another device: no remote copies, remote signals or barrier semaphores. Data moves between devices by JAX's collectives and lax.ppermute only.
A program may use at most 128 MiB of HBM per device.

```python
import math
import jax
import jax.numpy as jnp
from jax import lax

D = 2048
DR = 1024
BLK = 64
BLOCKS = 16
CONV = 4
H = 8
NOPE = 128
ROPE = 64
VH = 128
LAT = 512
DA = 1024
TOK_DEV = 256
SEQUENCE_LENGTH = 1024
N_TP = 2


def draw_decay_rate(key, part):
    pick_key, slow_key, fast_key = jax.random.split(key, 3)
    slow_share = 0.5
    slow_mask = jax.random.bernoulli(pick_key, slow_share, (DR,))
    slow_rate = jnp.exp(jax.random.uniform(slow_key, (DR,), jnp.float32, jnp.log(0.05), jnp.log(1.0))) / (8.0 * SEQUENCE_LENGTH)
    fast_rate = jnp.exp(jax.random.uniform(fast_key, (DR,), jnp.float32, jnp.log(0.004), jnp.log(0.012)))
    return jnp.where(slow_mask, slow_rate, fast_rate)


def draw_decay_shift(key, part):
    level_key, place_key, depth_key = jax.random.split(key, 3)
    block_count = SEQUENCE_LENGTH // TOK_DEV
    levels = jnp.exp(jax.random.uniform(level_key, (block_count,), jnp.float32, jnp.log(0.05), jnp.log(0.5))) / SEQUENCE_LENGTH
    baseline_offset = -jnp.repeat(levels, TOK_DEV)
    slot_indices = jax.random.randint(place_key, (2,), 0, SEQUENCE_LENGTH)
    layer_depths = jnp.log(jax.random.uniform(depth_key, (2,), jnp.float32, 0.5, 0.8))
    spike_flags = jnp.arange(SEQUENCE_LENGTH)[:, None] == slot_indices[None, :]
    return baseline_offset + jnp.sum(jnp.where(spike_flags, layer_depths[None, :], 0.0), axis=1)


def draw_query_gain(key, part):
    gain_key = jax.random.fold_in(key, 0)
    gain_values = jax.random.uniform(gain_key, (NOPE + ROPE,), jnp.float32, 0.4, 1.6)
    return gain_values


def level_of(rng, extent, cuts, least, high):
    level = 1.0
    for axis_at, parts in cuts:
        heights = jax.random.uniform(jax.random.fold_in(jax.random.fold_in(rng, 6), axis_at), (parts,), jnp.float32, least / len(cuts), high / len(cuts))
        level = level * jnp.repeat(jnp.exp(heights), extent[axis_at] // parts).reshape((-1,) + (1,) * (len(extent) - 1 - axis_at))
    return level


def scatter_about(key, extent, scale, bound, cuts=(), kind=jnp.bfloat16):
    array = scale * jax.random.normal(key, extent, jnp.float32)
    if cuts:
        array = array * level_of(key, extent, cuts, -0.22, 0.18)
    return jnp.clip(array, -bound, bound).astype(kind)


def setup_inputs(seed: int = 0, part: int = 0) -> dict:
    splits = jax.random.split(jax.random.key(seed), 20)
    part_keys = jax.random.split(jax.random.fold_in(splits[19], part), 20)
    return {
        "tokens": scatter_about(part_keys[0], (SEQUENCE_LENGTH, D), 1.0, 6.0, ((0, 8),)),
        "norm_gain": jnp.clip(1.0 + 0.18 * jax.random.normal(splits[1], (D,), jnp.float32), 0.1, 1.9),
        "recurrent_input": scatter_about(splits[2], (D, DR), D ** -0.5, 0.125, ((1, 2),)),
        "recurrent_gate": scatter_about(splits[3], (D, DR), D ** -0.5, 0.125, ((1, 2),)),
        "attention_gate": scatter_about(splits[4], (D, DA), D ** -0.5, 0.125, ((1, 2),)),
        "query_proj": scatter_about(splits[5], (D, H * (NOPE + ROPE)), D ** -0.5, 0.125, ((1, 2),)),
        "latent_down": scatter_about(splits[6], (D, LAT), D ** -0.5, 0.125, ((1, 2),)),
        "rope_key_down": scatter_about(splits[7], (D, ROPE), D ** -0.5, 0.125),
        "conv_kernel": scatter_about(splits[8], (CONV, DR), 0.5, 3.0, ((1, 2),), jnp.float32),
        "recurrence_gate_blocks": scatter_about(splits[9], (BLOCKS, BLK, BLK), BLK ** -0.5, 0.75, ((0, 2),)),
        "input_gate_blocks": scatter_about(splits[10], (BLOCKS, BLK, BLK), BLK ** -0.5, 0.75, ((0, 2),)),
        "decay_rate": draw_decay_rate(jax.random.fold_in(splits[19], 71), part),
        "decay_shift": draw_decay_shift(jax.random.fold_in(jax.random.fold_in(splits[19], part), 71), part),
        "initial_state": scatter_about(part_keys[13], (DR,), 1.0, 6.0, ((0, 2),), jnp.float32),
        "latent_gain": jnp.clip(1.0 + 0.18 * jax.random.normal(splits[14], (LAT,), jnp.float32), 0.1, 1.9),
        "latent_up": scatter_about(splits[15], (LAT, H * (NOPE + VH)), LAT ** -0.5, 0.25, ((1, 2),)),
        "query_gain": draw_query_gain(jax.random.fold_in(splits[19], 71), part),
        "recurrent_output": scatter_about(splits[17], (DR, D), ((DR + DA) // 4) ** -0.5, 0.25, ((0, 2),)),
        "attention_output": scatter_about(splits[18], (DA, D), ((DR + DA) // 4) ** -0.5, 0.25, ((0, 2),)),
    }


EPS = 1e-06
RECURRENT_SCALE = 8.0
THETA = 10000.0

def rotate_half(values, token_positions):
    half_width = values.shape[-1] // 2
    inv_freq = 1.0 / THETA ** (jnp.arange(0, 2 * half_width, 2, dtype=jnp.float32) / (2 * half_width))
    angles = token_positions.astype(jnp.float32)[:, None] * inv_freq[None, :]
    cosine = jnp.cos(angles)
    sine_part = jnp.sin(angles)
    if values.ndim == 3:
        cosine = cosine[:, None, :]
        sine_part = sine_part[:, None, :]
    first_half = values[..., :half_width]
    second_half = values[..., half_width:]
    return jnp.concatenate([first_half * cosine - second_half * sine_part, first_half * sine_part + second_half * cosine], axis=-1)

def rms_scaled(values, gain_vec):
    return values * lax.rsqrt(lax.optimization_barrier(jnp.mean(values * values, axis=-1, keepdims=True)) + EPS) * gain_vec

def rounded(values):
    return lax.optimization_barrier(values.astype(jnp.bfloat16)).astype(jnp.float32)

def linear_step(earlier, later_part):
    return (earlier[0] * later_part[0], later_part[0] * earlier[1] + later_part[1])

def reference(tokens, norm_gain, recurrent_input, recurrent_gate, attention_gate, query_proj, latent_down, rope_key_down, conv_kernel, recurrence_gate_blocks, input_gate_blocks, decay_rate, decay_shift, initial_state, latent_gain, latent_up, query_gain, recurrent_output, attention_output):
    normed = rms_scaled(tokens.astype(jnp.float32), norm_gain).astype(jnp.bfloat16)

    def project(weight):
        return jnp.dot(normed, weight, preferred_element_type=jnp.float32).astype(jnp.bfloat16)
    recur_signal = project(recurrent_input)
    recur_gate_pre = project(recurrent_gate)
    attention_pre = project(attention_gate)
    query_raw = project(query_proj)
    latent_raw = project(latent_down)
    rope_raw = project(rope_key_down)
    token_positions = jnp.arange(SEQUENCE_LENGTH, dtype=jnp.int32)
    padded = jnp.concatenate([jnp.zeros((CONV - 1, DR), jnp.bfloat16), recur_signal], axis=0).astype(jnp.float32)
    conv_sum = conv_kernel[0] * padded[0:SEQUENCE_LENGTH]
    for tap_index in range(1, CONV):
        conv_sum = conv_sum + conv_kernel[tap_index] * padded[tap_index:tap_index + SEQUENCE_LENGTH]
    conv_back = rounded(conv_sum)
    grouped = conv_back.reshape(SEQUENCE_LENGTH, BLOCKS, BLK)
    recur_rate = jax.nn.sigmoid(jnp.einsum('tbi,bij->tbj', grouped, recurrence_gate_blocks.astype(jnp.float32)).reshape(SEQUENCE_LENGTH, DR))
    input_rate = jax.nn.sigmoid(jnp.einsum('tbi,bij->tbj', grouped, input_gate_blocks.astype(jnp.float32)).reshape(SEQUENCE_LENGTH, DR))
    log_decay = -RECURRENT_SCALE * recur_rate * decay_rate + decay_shift[:, None]
    decay = jnp.exp(log_decay)
    driven = jnp.sqrt(-jnp.expm1(2.0 * log_decay)) * input_rate * conv_back
    driven = driven.at[0].add(decay[0] * initial_state)
    decay_prod, states = lax.associative_scan(linear_step, (decay, driven), axis=0)
    recur_out = (states * jax.nn.silu(recur_gate_pre.astype(jnp.float32))).astype(jnp.bfloat16)
    query_rows = rms_scaled(query_raw.astype(jnp.float32).reshape(SEQUENCE_LENGTH, H, NOPE + ROPE), query_gain)
    query_rows = jnp.concatenate([query_rows[..., :NOPE], rotate_half(query_rows[..., NOPE:], token_positions)], axis=-1).astype(jnp.bfloat16)
    latent = rms_scaled(latent_raw.astype(jnp.float32), latent_gain).astype(jnp.bfloat16)
    key_values = jnp.dot(latent, latent_up, preferred_element_type=jnp.float32).astype(jnp.bfloat16).reshape(SEQUENCE_LENGTH, H, NOPE + VH)
    key_nope = key_values[..., :NOPE].astype(jnp.float32)
    values_all = key_values[..., NOPE:].astype(jnp.float32)
    key_rope = rotate_half(rope_raw.astype(jnp.float32), token_positions).astype(jnp.bfloat16).astype(jnp.float32)
    query_block = math.gcd(SEQUENCE_LENGTH, 512)
    score_scale = (NOPE + ROPE) ** (-0.5)

    def attend(block_index):
        begin_row = (block_index * query_block).astype(jnp.int32)
        query_part = lax.dynamic_slice_in_dim(query_rows, begin_row, query_block, 0).astype(jnp.float32)
        scores = jnp.einsum('thd,khd->htk', query_part[..., :NOPE], key_nope)
        scores = scores + jnp.einsum('thr,kr->htk', query_part[..., NOPE:], key_rope)
        scores = scores * score_scale
        query_pos = begin_row + jnp.arange(query_block, dtype=jnp.int32)
        allowed = token_positions[None, None, :] <= query_pos[None, :, None]
        scores = jnp.where(allowed, scores, -jnp.inf)
        row_max = lax.optimization_barrier(jnp.max(scores, axis=-1, keepdims=True))
        weights = jnp.exp(scores - row_max)
        denominator = lax.optimization_barrier(jnp.sum(weights, axis=-1))
        weighted = jnp.einsum('htk,khd->thd', rounded(weights), values_all)
        return weighted / jnp.transpose(denominator)[:, :, None]
    attended = lax.map(attend, jnp.arange(SEQUENCE_LENGTH // query_block, dtype=jnp.int32)).reshape(SEQUENCE_LENGTH, DA)
    attention_out = (attended * jax.nn.silu(attention_pre.astype(jnp.float32))).astype(jnp.bfloat16)
    recur_group = DR // N_TP
    attend_group = DA // N_TP

    def add_group(group_index, running):
        index_value = group_index.astype(jnp.int32)
        recur_part = lax.dynamic_slice_in_dim(recur_out, index_value * recur_group, recur_group, 1)
        recur_rows = lax.dynamic_slice_in_dim(recurrent_output, index_value * recur_group, recur_group, 0)
        attend_part = lax.dynamic_slice_in_dim(attention_out, index_value * attend_group, attend_group, 1)
        attend_rows = lax.dynamic_slice_in_dim(attention_output, index_value * attend_group, attend_group, 0)
        partial_sum = jnp.dot(recur_part, recur_rows, preferred_element_type=jnp.float32) + jnp.dot(attend_part, attend_rows, preferred_element_type=jnp.float32)
        return running + rounded(partial_sum)
    total = lax.fori_loop(0, N_TP, add_group, jnp.zeros((SEQUENCE_LENGTH, D), jnp.float32))
    return total.astype(jnp.bfloat16)
```

```python
import functools
import math

import jax
import jax.numpy as jnp
from jax import lax
from jax.experimental import pallas as pl
from jax.experimental.pallas import tpu as pltpu
from jax.sharding import PartitionSpec as P

EPS = 1e-06
RECURRENT_SCALE = 8.0
THETA = 10000.0
LANES = 128
RIM = 8
F32 = jnp.float32
BF16 = jnp.bfloat16


def shifted(block, axis, distance):
    size = lax.axis_size(axis)
    return lax.ppermute(block, axis, [(i, i + distance) for i in range(size - distance)])


def others(block, axis):
    size = lax.axis_size(axis)
    if size == 1:
        return (block,)
    if size == 2:
        return (block, lax.ppermute(block, axis, [(0, 1), (1, 0)]))
    return tuple(lax.all_gather(block, axis)[i] for i in range(size))


def ordered(parts, place):
    if len(parts) != 2:
        return list(parts)
    first = place == 0
    return [jnp.where(first, parts[0], parts[1]), jnp.where(first, parts[1], parts[0])]


def pack(values):
    rows, width = values.shape
    if width >= LANES:
        return [values[:, i : i + LANES] for i in range(0, width, LANES)]
    groups = LANES // width
    step = rows // groups
    return [jnp.concatenate([values[g * step : (g + 1) * step] for g in range(groups)], axis=1)]


def unpack(packed, rows, width):
    if width >= LANES:
        return jnp.concatenate(
            [packed[i * rows : (i + 1) * rows] for i in range(width // LANES)], axis=1
        )
    groups = LANES // width
    return jnp.concatenate([packed[:, g * width : (g + 1) * width] for g in range(groups)], axis=0)


def rms(values, gain):
    return values * lax.rsqrt(jnp.mean(values * values, axis=-1, keepdims=True) + EPS) * gain


def dot(a, b):
    return jnp.dot(a, b, preferred_element_type=F32)


def rotated(values, table):
    half = values.shape[-1] // 2
    width = values.shape[-1]
    flipped = jnp.concatenate([values[:, half:], values[:, :half]], axis=1)
    return values * table[:, :width] + flipped * table[:, width : 2 * width]


def one_minus_exp(y):
    series = 1.0 - y * (1.0 / 8.0)
    for k in (7, 6, 5, 4, 3, 2):
        series = 1.0 - y * (1.0 / k) * series
    return jnp.where(y < 0.5, y * series, 1.0 - jnp.exp(-y))


def scan_rows(decay, driven):
    rows, width = decay.shape
    step = 1
    while step < rows:
        one = jnp.ones((step, width), F32)
        zero = jnp.zeros((step, width), F32)
        driven = driven + decay * jnp.concatenate([zero, driven[:-step]], axis=0)
        decay = decay * jnp.concatenate([one, decay[:-step]], axis=0)
        step *= 2
    return decay, driven


def front_kernel(dims, *refs):
    (tp_count, rows, share) = dims
    n_tok = 2 if tp_count == 2 else 1
    tok_refs = refs[:n_tok]
    (rim_ref, gain_ref, wl_ref, wr_ref, wi_ref, conv_ref, gb_ref, ib_ref, rate_ref, shift_ref,
     table_ref, normed_ref, send_ref, prod_ref, zero_ref, ext_ref) = refs[n_tok:]
    tp_place = lax.axis_index("tp")
    gain = gain_ref[...]
    ext_ref[0:RIM] = jnp.zeros((RIM, ext_ref.shape[1]), BF16)
    rim = rms(rim_ref[...].astype(F32), gain).astype(BF16)
    if n_tok == 2:
        for i, ref in enumerate(tok_refs):
            place = tp_place if i == 0 else 1 - tp_place
            normed_ref[pl.ds(pl.multiple_of(place * share, share), share), :] = rms(
                ref[...].astype(F32), gain
            ).astype(BF16)
    else:
        normed_ref[...] = rms(tok_refs[0][...].astype(F32), gain).astype(BF16)
    normed = normed_ref[...]
    latent = dot(normed, wl_ref[...]).astype(BF16)
    at = 0
    for piece in pack(latent):
        send_ref[at : at + piece.shape[0]] = piece
        at += piece.shape[0]
    begin = pl.multiple_of(tp_place * share, share)
    rope = dot(normed_ref[pl.ds(begin, share), :], wr_ref[...]).astype(BF16).astype(F32)
    rope = rotated(rope, table_ref[pl.ds(begin, share), :]).astype(BF16)
    for piece in pack(rope):
        send_ref[at : at + piece.shape[0]] = piece
        at += piece.shape[0]
    signal = dot(normed, wi_ref[...]).astype(BF16).astype(F32)
    before = dot(rim, wi_ref[...]).astype(BF16).astype(F32)
    extended = jnp.concatenate([before, signal], axis=0)
    taps = conv_ref.shape[0]
    first = RIM - taps + 1
    conv_sum = conv_ref[0:1, :] * extended[first : first + rows]
    for tap in range(1, taps):
        conv_sum = conv_sum + conv_ref[tap : tap + 1, :] * extended[first + tap : first + tap + rows]
    conv_out = conv_sum.astype(BF16)
    block = gb_ref.shape[1]
    group = LANES // block
    pre_r, pre_i = [], []
    for base in range(0, gb_ref.shape[0], group):
        lhs = conv_out[:, base * block : (base + group) * block]
        for ref, into in ((gb_ref, pre_r), (ib_ref, pre_i)):
            bands = []
            for g in range(group):
                cells = [jnp.zeros((block, block), BF16)] * group
                cells[g] = ref[base + g]
                bands.append(jnp.concatenate(cells, axis=1))
            into.append(dot(lhs, jnp.concatenate(bands, axis=0)))
    recur_rate = jax.nn.sigmoid(jnp.concatenate(pre_r, axis=1))
    input_rate = jax.nn.sigmoid(jnp.concatenate(pre_i, axis=1))
    log_decay = -RECURRENT_SCALE * recur_rate * rate_ref[...] + shift_ref[...]
    decay = jnp.exp(log_decay)
    driven = jnp.sqrt(one_minus_exp(-2.0 * log_decay)) * input_rate * conv_out.astype(F32)
    prod, zero = scan_rows(decay, driven)
    prod_ref[...] = prod
    zero_ref[...] = zero
    carries = []
    for value in (prod[rows - 1 : rows], zero[rows - 1 : rows]):
        high = value.astype(BF16)
        carries += [high, (value - high.astype(F32)).astype(BF16)]
    lines = []
    for value in carries:
        lines += [value[:, i : i + LANES] for i in range(0, value.shape[1], LANES)]
    pad = send_ref.shape[0] - at - len(lines)
    if pad:
        lines.append(jnp.zeros((pad, LANES), BF16))
    send_ref[at:] = jnp.concatenate(lines, axis=0)


def middle_kernel(head_dim, normed_ref, wg_ref, wa_ref, wq_ref, gain_ref, table_ref, gr_ref, ga_ref, q_ref):
    normed = normed_ref[...]
    rope_width = table_ref.shape[1] // 2
    nope = head_dim - rope_width
    raw = dot(normed, wq_ref[...]).astype(BF16).astype(F32)
    table = table_ref[...]
    for head in range(q_ref.shape[0]):
        q = rms(raw[:, head * head_dim : (head + 1) * head_dim], gain_ref[...])
        q = jnp.concatenate([q[:, :nope], rotated(q[:, nope:], table)], axis=1)
        q_ref[head] = q.astype(BF16)
    gr_ref[...] = dot(normed, wg_ref[...]).astype(BF16)
    ga_ref[...] = dot(normed, wa_ref[...]).astype(BF16)


def attend_kernel(dims, *refs):
    (distance, n_parts, rows, latent_width, share, rope_width, vh) = dims
    part_refs = refs[:n_parts]
    refs = refs[n_parts:]
    if distance:
        q_ref, gain_ref, up_ref, acc_in, ml_in, acc_ref, ml_ref = refs
    else:
        q_ref, gain_ref, up_ref, acc_ref, ml_ref = refs
    heads, q_rows, head_dim = q_ref.shape
    nope = head_dim - rope_width
    factor = head_dim ** (-0.5) * math.log2(math.e)

    def run():
        parts = ordered([ref[...] for ref in part_refs], lax.axis_index("tp"))
        lat_rows = rows * latent_width // LANES
        rope_rows = share * rope_width // LANES
        latent = jnp.concatenate([unpack(p[:lat_rows], rows, latent_width) for p in parts], axis=1)
        rope = jnp.concatenate(
            [unpack(p[lat_rows : lat_rows + rope_rows], share, rope_width) for p in parts], axis=0
        )
        latent = rms(latent.astype(F32), gain_ref[...]).astype(BF16)
        expanded = dot(latent, up_ref[...]).astype(BF16)
        if not distance:
            allowed = lax.broadcasted_iota(jnp.int32, (q_rows, rows), 1) <= lax.broadcasted_iota(
                jnp.int32, (q_rows, rows), 0
            )
        tails = []
        for head in range(heads):
            base = head * (nope + vh)
            key = jnp.concatenate([expanded[:, base : base + nope], rope], axis=1)
            value = expanded[:, base + nope : base + nope + vh]
            scores = lax.dot_general(
                q_ref[head], key, (((1,), (1,)), ((), ())), preferred_element_type=F32
            )
            if not distance:
                scores = jnp.where(allowed, scores, -jnp.inf)
            top = jnp.max(scores, axis=-1, keepdims=True)
            if distance:
                old = ml_in[:, head : head + 1]
                top = jnp.maximum(top, old)
            weights = jnp.exp2((scores - top) * factor)
            total = jnp.sum(weights, axis=-1, keepdims=True)
            out = dot(weights.astype(BF16), value)
            span = slice(head * vh, (head + 1) * vh)
            if distance:
                scale = jnp.exp2((old - top) * factor)
                total = total + scale * ml_in[:, heads + head : heads + head + 1]
                out = out + scale * acc_in[:, span]
            acc_ref[:, span] = out
            ml_ref[:, head : head + 1] = top
            ml_ref[:, heads + head : heads + head + 1] = total

    if distance:
        valid = lax.axis_index("sp") >= distance
        pl.when(valid)(run)

        @pl.when(jnp.logical_not(valid))
        def _():
            acc_ref[...] = acc_in[...]
            ml_ref[...] = ml_in[...]
    else:
        run()


def back_kernel(dims, *refs):
    (n_carry, carry_at, heads, half, share, mine) = dims
    carry_refs = refs[:n_carry]
    (init_ref, prod_ref, zero_ref, gr_ref, ga_ref, acc_ref, ml_ref, wr_ref, wa_ref, out_ref) = refs[n_carry:]
    sp_place = lax.axis_index("sp")
    state = init_ref[...]
    width = state.shape[1]
    lines = width // LANES

    def vector(tile, k):
        return jnp.concatenate(
            [tile[k * lines + i : k * lines + i + 1] for i in range(lines)], axis=1
        )

    for distance in range(n_carry, 0, -1):
        tile = carry_refs[distance - 1][carry_at:].astype(F32)
        decay = vector(tile, 0) + vector(tile, 1)
        driven = vector(tile, 2) + vector(tile, 3)
        state = jnp.where(distance <= sp_place, decay * state + driven, state)
    if half:
        place = lax.axis_index("tp")
        place = place if mine else 1 - place
        span = pl.ds(pl.multiple_of(place * share, share), share)
    else:
        span = slice(None)
    states = zero_ref[span, :] + prod_ref[span, :] * state
    recur = (states * jax.nn.silu(gr_ref[span, :].astype(F32))).astype(BF16)
    totals = ml_ref[span, :]
    acc = acc_ref[span, :]
    vh = acc.shape[1] // heads
    attended = jnp.concatenate(
        [
            acc[:, h * vh : (h + 1) * vh] / totals[:, heads + h : heads + h + 1]
            for h in range(heads)
        ],
        axis=1,
    )
    attended = (attended * jax.nn.silu(ga_ref[span, :].astype(F32))).astype(BF16)
    out_ref[...] = (dot(recur, wr_ref[...]) + dot(attended, wa_ref[...])).astype(BF16)


def call(kernel, out_shape, args, flops, name, scratch=()):
    return pl.pallas_call(
        kernel,
        out_shape=out_shape,
        scratch_shapes=list(scratch),
        name=name,
        cost_estimate=pl.CostEstimate(flops=flops, transcendentals=0, bytes_accessed=1 << 20),
        compiler_params=pltpu.CompilerParams(vmem_limit_bytes=40 << 20),
    )(*args)


def body(
    tokens,
    norm_gain,
    recurrent_input,
    recurrent_gate,
    attention_gate,
    query_proj,
    latent_down,
    rope_key_down,
    conv_kernel,
    recurrence_gate_blocks,
    input_gate_blocks,
    decay_rate,
    decay_shift,
    initial_state,
    latent_gain,
    latent_up,
    query_gain,
    recurrent_output,
    attention_output,
):
    tp_count = lax.axis_size("tp")
    sp_count = lax.axis_size("sp")
    sp_place = lax.axis_index("sp")
    share, model = tokens.shape
    rows = share * tp_count
    channels = recurrent_input.shape[1]
    latent_width = latent_down.shape[1]
    rope_width = rope_key_down.shape[1]
    head_dim = query_gain.shape[0]
    heads = query_proj.shape[1] // head_dim
    vh = attention_gate.shape[1] // heads

    if tp_count == 2:
        token_parts = others(tokens, "tp")
        last = jnp.concatenate([tokens[share - RIM :]], axis=0)
        n = sp_count
        straight = lax.ppermute(
            last, ("sp", "tp"), [(2 * i + 1, 2 * i + 3) for i in range(n - 1)]
        )
        crossed = lax.ppermute(
            last, ("sp", "tp"), [(2 * i + 1, 2 * i + 2) for i in range(n - 1)]
        )
        rim = straight + crossed
    else:
        token_parts = (lax.all_gather(tokens, "tp", axis=0, tiled=True),)
        rim = shifted(token_parts[0][rows - RIM :], "sp", 1)

    half = rope_width // 2
    inv_freq = 1.0 / THETA ** (jnp.arange(0, rope_width, 2, dtype=F32) / rope_width)
    positions = (sp_place * rows + jnp.arange(rows, dtype=jnp.int32)).astype(F32)
    angles = positions[:, None] * jnp.tile(inv_freq, 4)[None, :]
    lane = jnp.arange(4 * half)[None, :]
    sine = jnp.sin(angles)
    table = jnp.where(lane < 2 * half, jnp.cos(angles), jnp.where(lane < 3 * half, -sine, sine))

    lat_rows = rows * latent_width // LANES
    rope_rows = share * rope_width // LANES
    carry_rows = -(-4 * channels // LANES // 16) * 16
    send_rows = lat_rows + rope_rows + carry_rows
    sds = jax.ShapeDtypeStruct
    normed, send, prod, zero = call(
        functools.partial(front_kernel, (tp_count, rows, share)),
        (
            sds((rows, model), BF16),
            sds((send_rows, LANES), BF16),
            sds((rows, channels), F32),
            sds((rows, channels), F32),
        ),
        (
            *token_parts,
            rim,
            norm_gain[None],
            latent_down,
            rope_key_down,
            recurrent_input,
            conv_kernel,
            recurrence_gate_blocks,
            input_gate_blocks,
            decay_rate[None],
            decay_shift[:, None],
            table,
        ),
        2 * rows * model * (latent_width + channels),
        "front",
        [pltpu.VMEM((rows + RIM, LANES), BF16)],
    )
    blocks = [send] + [shifted(send, "sp", d) for d in range(1, sp_count)]

    gate_r, gate_a, query = call(
        functools.partial(middle_kernel, head_dim),
        (
            sds((rows, channels), BF16),
            sds((rows, heads * vh), BF16),
            sds((heads, rows, head_dim), BF16),
        ),
        (normed, recurrent_gate, attention_gate, query_proj, query_gain[None], table),
        2 * rows * model * (channels + heads * (vh + head_dim)),
        "middle",
    )
    state = ()
    for distance, block in enumerate(blocks):
        parts = others(block, "tp")
        state = call(
            functools.partial(
                attend_kernel, (distance, len(parts), rows, latent_width, share, rope_width, vh)
            ),
            (sds((rows, heads * vh), F32), sds((rows, LANES), F32)),
            (*parts, query, latent_gain[None], latent_up, *state),
            2 * rows * (latent_up.shape[0] * latent_up.shape[1] + rows * heads * (head_dim + vh)),
            f"attend{distance}",
        )
    acc, ml = state

    def back(halved, mine):
        return call(
            functools.partial(
                back_kernel, (sp_count - 1, lat_rows + rope_rows, heads, halved, share, mine)
            ),
            sds((share if halved else rows, model), BF16),
            (
                *blocks[1:],
                initial_state[None],
                prod,
                zero,
                gate_r,
                gate_a,
                acc,
                ml,
                recurrent_output,
                attention_output,
            ),
            2 * (share if halved else rows) * model * (channels + heads * vh),
            "back_mine" if mine else "back_theirs",
        )

    if tp_count == 2:
        theirs = back(True, False)
        arrived = lax.ppermute(theirs, "tp", [(0, 1), (1, 0)])
        mine = back(True, True)
        return (arrived.astype(F32) + mine.astype(F32)).astype(BF16)
    return lax.psum_scatter(back(False, True), "tp", scatter_dimension=0, tiled=True)


def solution(mesh):
    return jax.shard_map(
        body,
        mesh=mesh,
        in_specs=(
            P(("fs", "sp", "tp"), None),
            P(),
            P(None, "tp"),
            P(None, "tp"),
            P(None, "tp"),
            P(None, "tp"),
            P(None, "tp"),
            P(),
            P(None, "tp"),
            P("tp", None, None),
            P("tp", None, None),
            P("tp"),
            P(("fs", "sp")),
            P(("fs", "tp")),
            P(),
            P(None, "tp"),
            P(),
            P("tp", None),
            P("tp", None),
        ),
        out_specs=P(("fs", "sp", "tp"), None),
        check_vma=False,
    )
```
